32 devices in a mesh: sp: 16 (over z, y, x), tp: 2 (over core).
Axes of the slice: x: 2, y: 2, z: 4, core: 2. Of those that a mesh axis runs over, the one named last changes fastest.
Arguments:
- prompt: bfloat16 [2, 3072, 4096], P(None, 'sp'), as said below
- w_key: bfloat16 [4096, 2048], P('sp', 'tp'), may hold values from -0.09375 to 0.09375
- w_value: bfloat16 [4096, 4096], P('sp', 'tp'), may hold values from -0.09375 to 0.09375
- w_igate: bfloat16 [4096, 8], replicated, may hold values from -0.09375 to 0.09375
- w_fgate: bfloat16 [4096, 8], replicated, may hold values from -0.09375 to 0.09375
- input_bias: float32 [8], replicated, may hold values from -1 to 120
- forget_bias: float32 [8], replicated, may hold values from 4 to 20
- new_query: bfloat16 [2, 8, 256], P(None, 'tp'), may hold values from -6 to 6
- new_key: bfloat16 [2, 8, 256], P(None, 'tp'), may hold values from -6 to 6
- new_value: bfloat16 [2, 8, 512], P(None, 'tp'), may hold values from -6 to 6
- new_gates: float32 [2, 2, 8], P(None, None, 'tp'), may hold values from 2 to 9
Outputs:
- cache_memory: bfloat16 [2, 8, 256, 512], P(None, 'tp', 'sp')
- cache_norm: float32 [2, 8, 256], P(None, 'tp', 'sp')
- cache_max: float32 [2, 8], P(None, 'tp')
- first_read: bfloat16 [2, 8, 512], P(None, 'tp')
The draws below stay inside these ranges and needn't reach their ends.
Inputs may be any that keep to these rules, and one draw needn't show every extreme that they name: `prompt`: Real-valued features, each entry drawn independently; their magnitude differs from one block of 192 positions to the next.
All inputs are finite; a program needn't handle non-finite values.
Results may differ from the reference program's by a relative error of at most 0.019.
Values may be sent and summed in bfloat16 or wider, within the bound.
No kernel may reach another device: no remote copies, remote signals or barrier semaphores. Data moves between devices by JAX's collectives and lax.ppermute only.
A program may use at most 64 MiB of HBM per device.

```python
import math
import jax
import jax.numpy as jnp
from jax import lax

D = 4096
HEADS = 8
DK = 256
DV = 512
SEQS = 2
SPAN = 192
LEN = 3072


def draw_prompt(key, part):
    first, second = jax.random.split(jax.random.fold_in(key, 11))
    base = jax.random.normal(first, (SEQS, LEN // SPAN, SPAN, D), jnp.float32)
    lower, upper = (0.6, 1.7)
    scales = jnp.exp(jax.random.uniform(second, (SEQS, LEN // SPAN, 1, 1), jnp.float32, math.log(lower), math.log(upper)))
    return (base * scales).reshape(SEQS, LEN, D).astype(jnp.bfloat16)


def draw_input_bias(key, part):
    inner = jax.random.fold_in(key, 23)
    return jax.random.uniform(inner, (HEADS,), jnp.float32, -1.0, 1.0)


def draw_forget_bias(key, part):
    first, second, third = jax.random.split(jax.random.fold_in(key, 37), 3)
    picks = jax.random.randint(first, (HEADS,), 0, 8)
    quick = picks < 4
    slow_value = math.log(float(LEN)) + jax.random.uniform(second, (HEADS,), jnp.float32, 1.5, 2.5)
    quick_value = jax.random.uniform(third, (HEADS,), jnp.float32, 4.0, 5.0)
    return jnp.where(quick, quick_value, slow_value)


def shard_levels(own_key, dims, cuts, least, top_value):
    level = 1.0
    for position, parts in cuts:
        heights = jax.random.uniform(jax.random.fold_in(jax.random.fold_in(own_key, 6), position), (parts,), jnp.float32, least / len(cuts), top_value / len(cuts))
        level = level * jnp.repeat(jnp.exp(heights), dims[position] // parts).reshape((-1,) + (1,) * (len(dims) - 1 - position))
    return level


def normal_values(own_key, dims, deviation, limit, shards=(), held_as=jnp.bfloat16):
    result = deviation * jax.random.normal(own_key, dims, jnp.float32)
    if shards:
        result = result * shard_levels(own_key, dims, shards, -0.22, 0.18)
    return jnp.clip(result, -limit, limit).astype(held_as)


def setup_inputs(seed: int = 0) -> dict:
    key_list = jax.random.split(jax.random.key(seed), 12)
    prompt = draw_prompt(jax.random.fold_in(key_list[11], 71), 0)
    w_key = normal_values(key_list[1], (D, HEADS * DK), D ** -0.5, 0.09375, ((0, 16), (1, 2)))
    w_value = normal_values(key_list[2], (D, HEADS * DV), D ** -0.5, 0.09375, ((0, 16), (1, 2)))
    w_igate = normal_values(key_list[3], (D, HEADS), D ** -0.5, 0.09375)
    w_fgate = normal_values(key_list[4], (D, HEADS), D ** -0.5, 0.09375)
    input_bias = draw_input_bias(jax.random.fold_in(key_list[11], 71), 0)
    forget_bias = draw_forget_bias(jax.random.fold_in(key_list[11], 71), 0)
    new_query = normal_values(key_list[7], (SEQS, HEADS, DK), 1.0, 6.0, ((1, 2),))
    new_key = normal_values(key_list[8], (SEQS, HEADS, DK), 1.0, 6.0, ((1, 2),))
    new_value = normal_values(key_list[9], (SEQS, HEADS, DV), 1.0, 6.0, ((1, 2),))
    new_gates = jnp.clip(2.0 + 7.0 * jax.random.uniform(key_list[10], (2, SEQS, HEADS), jnp.float32) ** shard_levels(key_list[10], (2, SEQS, HEADS), ((2, 2),), -0.2, 0.2), 2.0, 9.0)
    return {"prompt": prompt, "w_key": w_key, "w_value": w_value, "w_igate": w_igate, "w_fgate": w_fgate, "input_bias": input_bias, "forget_bias": forget_bias, "new_query": new_query, "new_key": new_key, "new_value": new_value, "new_gates": new_gates}


def reference(prompt, w_key, w_value, w_igate, w_fgate, input_bias, forget_bias, new_query, new_key, new_value, new_gates):
    blocks = LEN // SPAN
    token_rows = prompt.reshape(SEQS * LEN, D)
    key_rows = jnp.dot(token_rows, w_key, preferred_element_type=jnp.float32).astype(jnp.bfloat16)
    value_rows = jnp.dot(token_rows, w_value, preferred_element_type=jnp.float32).astype(jnp.bfloat16)
    input_gate = jnp.dot(token_rows, w_igate, preferred_element_type=jnp.float32) + input_bias
    log_forget = jax.nn.log_sigmoid(jnp.dot(token_rows, w_fgate, preferred_element_type=jnp.float32) + forget_bias)
    input_gate = input_gate.reshape(SEQS, blocks, SPAN, HEADS)
    log_forget = log_forget.reshape(SEQS, blocks, SPAN, HEADS)
    block_total = jnp.sum(log_forget, axis=2)
    forget_after = block_total[:, :, None] - jnp.cumsum(log_forget, axis=2)
    log_weight = forget_after + input_gate
    block_max = jnp.max(log_weight, axis=2)
    later_total = jnp.flip(jnp.cumsum(jnp.flip(block_total, 1), axis=1), 1) - block_total
    block_lift = later_total + block_max
    global_max = jnp.max(block_lift, axis=1)
    factor = jnp.exp(block_lift - global_max[:, None])
    key_scale = DK ** -0.5
    key_blocks = key_rows.reshape(SEQS, blocks, SPAN, HEADS, DK).astype(jnp.float32)
    decayed = (jnp.exp(log_weight - block_max[:, :, None])[..., None] * key_scale * key_blocks).astype(jnp.bfloat16)
    value_blocks = value_rows.reshape(SEQS, blocks, SPAN, HEADS, DV)

    def accumulate(carry, inputs):
        memory, normal = carry
        block_keys, block_values, block_factor = inputs
        block_state = jnp.einsum('sthk,sthv->shkv', block_keys.astype(jnp.float32), block_values.astype(jnp.float32),
                                 precision=lax.Precision.HIGHEST)
        block_norm = jnp.sum(block_keys.astype(jnp.float32), axis=1)
        memory = memory + block_factor[:, :, None, None] * block_state
        normal = normal + block_factor[:, :, None] * block_norm
        return (memory, normal), None

    inputs = (jnp.moveaxis(decayed, 1, 0), jnp.moveaxis(value_blocks, 1, 0), jnp.moveaxis(factor, 1, 0))
    start = (jnp.zeros((SEQS, HEADS, DK, DV), jnp.float32), jnp.zeros((SEQS, HEADS, DK), jnp.float32))
    (memory, normal), _ = lax.scan(accumulate, start, inputs)
    query_full = new_query.astype(jnp.float32)
    query_state = jnp.einsum('shk,shkv->shv', query_full, memory, precision=lax.Precision.HIGHEST)
    query_norm = jnp.sum(query_full * normal, axis=-1)
    forget_new = jax.nn.log_sigmoid(new_gates[1])
    input_new = new_gates[0]
    mixed = jnp.maximum(forget_new + global_max, input_new)
    carried = jnp.exp(forget_new + global_max - mixed)
    fresh = jnp.exp(input_new - mixed)
    own_score = jnp.sum(query_full * new_key.astype(jnp.float32), axis=-1) * key_scale
    numer = carried[..., None] * query_state + (fresh * own_score)[..., None] * new_value.astype(jnp.float32)
    denom = carried * query_norm + fresh * own_score
    first_read = (numer / jnp.maximum(jnp.abs(denom), 1.0)[..., None]).astype(jnp.bfloat16)
    return memory.astype(jnp.bfloat16), normal, global_max, first_read
```

```python
import jax
import jax.numpy as jnp
from jax import lax
from jax.sharding import PartitionSpec as P


def swap(value, mask, count):
    return lax.ppermute(value, "sp", [(i, i ^ mask) for i in range(count)])


def swap_core(value):
    cores = lax.axis_size("tp")
    return lax.ppermute(value, "tp", [(i, cores - 1 - i) for i in range(cores)])


def offsets_of(masks):
    found = [0]
    for mask in masks:
        found = found + [off ^ mask for off in found]
    return found


def spread(value, masks, count):
    held = {0: value}
    for mask in masks:
        for off in list(held):
            held[off ^ mask] = swap(held[off], mask, count)
    return held


def plan(count, heads):
    bits = count.bit_length() - 1
    head_bits = heads.bit_length() - 1
    masks = [1 << b for b in range(bits)]
    preferred = [1 << b for b in range(0, bits, 2)] + [1 << b for b in range(1, bits, 2)]
    head_masks = sorted(preferred[:head_bits])
    token_masks = [m for m in masks if m not in head_masks]
    return head_masks, token_masks


def packed(index, masks):
    total = 0
    for place, mask in enumerate(masks):
        total = total + ((index // mask) % 2) * (1 << place)
    return total


def per_device(
    prompt,
    w_key,
    w_value,
    w_igate,
    w_fgate,
    input_bias,
    forget_bias,
    new_query,
    new_key,
    new_value,
    new_gates,
):
    count = lax.axis_size("sp")
    me = lax.axis_index("sp")
    core = lax.axis_index("tp")
    seqs, span, width = prompt.shape
    heads, key_size = new_query.shape[1:]
    value_size = new_value.shape[2]
    key_scale = key_size ** (-0.5)
    head_masks, token_masks = plan(count, heads)
    head_offs = offsets_of(head_masks)
    my_head = packed(me, head_masks)
    bits = count.bit_length() - 1

    def head_at(off):
        return packed(me ^ off, head_masks)

    depth = w_key.shape[0]
    both = key_size + value_size

    def columns(head):
        keys = lax.dynamic_slice_in_dim(w_key, head * key_size, key_size, 1)
        values = lax.dynamic_slice_in_dim(w_value, head * value_size, value_size, 1)
        return jnp.concatenate([keys, values], axis=1)

    group = jnp.zeros((len(head_offs), depth, both), jnp.bfloat16)
    for off in head_offs:
        piece = columns(head_at(off))
        if off:
            piece = swap(piece, off, count)
        group = lax.dynamic_update_slice(group, piece[None], (head_at(off), 0, 0))
    groups = spread(group, token_masks[::-1], count)

    rows = prompt.reshape(seqs * span, width)
    shared = lax.axis_size("tp") == 2
    half = seqs * span // 2
    mine = lax.dynamic_slice_in_dim(rows, core * half, half, 0) if shared else rows
    halves = spread(mine, head_masks[::-1], count)
    features = {0: rows}
    for off in head_offs[1:]:
        if not shared:
            features[off] = halves[off]
            continue
        other = swap_core(halves[off])
        first = jnp.where(core == 0, halves[off], other)
        second = jnp.where(core == 0, other, halves[off])
        features[off] = jnp.concatenate([first, second], axis=0)

    w_gates = jnp.concatenate([w_igate, w_fgate], axis=1)
    all_heads = w_igate.shape[1]
    before = (
        lax.broadcasted_iota(jnp.int32, (span, span), 0)
        >= lax.broadcasted_iota(jnp.int32, (span, span), 1)
    ).astype(jnp.float32)

    def gates(piece):
        raw = jnp.dot(piece, w_gates, preferred_element_type=jnp.float32)
        log_in = raw[:, :all_heads] + input_bias
        log_forget = jax.nn.log_sigmoid(raw[:, all_heads:] + forget_bias)
        log_in = lax.dynamic_slice_in_dim(log_in, core * heads, heads, 1)
        log_forget = lax.dynamic_slice_in_dim(log_forget, core * heads, heads, 1)
        log_in = log_in.reshape(seqs, span, heads)
        log_forget = log_forget.reshape(seqs, span, heads)
        total = jnp.sum(log_forget, axis=1)
        running = jnp.einsum(
            "ut,sth->suh", before, log_forget, precision=lax.Precision.HIGHEST
        )
        return total, total[:, None] - running + log_in

    total, log_weight = gates(rows)
    stats = jnp.stack([total, jnp.max(log_weight, axis=1)])
    table = jnp.zeros((count,) + stats.shape, jnp.float32)
    table = lax.dynamic_update_slice(table, stats[None], (me, 0, 0, 0))
    for mask in token_masks + head_masks:
        table = table + swap(table, mask, count)
    totals, maxima = table[:, 0], table[:, 1]
    later = jnp.flip(jnp.cumsum(jnp.flip(totals, 0), axis=0), 0) - totals
    cache_max = jnp.max(later + maxima, axis=0)
    shift = later - cache_max

    whole = jnp.zeros((count, depth, both), jnp.bfloat16)
    for token_off, piece in groups.items():
        for place, off in enumerate(head_offs):
            source = sum(((place // (1 << b)) % 2) * m for b, m in enumerate(head_masks))
            base = sum(m * (((me ^ token_off) // m) % 2) for m in token_masks)
            whole = lax.dynamic_update_slice(
                whole, piece[place][None], (base + source, 0, 0)
            )
    whole = whole.reshape(count * depth, both)

    decayed_all, value_all = [], []
    for off in head_offs:
        piece = features[off]
        if off:
            _, log_weight = gates(piece)
        block = me ^ off
        factor = lax.dynamic_slice_in_dim(shift, block, 1, 0)[0]
        weight = jnp.exp(log_weight + factor[:, None])
        weight = lax.dynamic_slice_in_dim(weight, my_head, 1, 2)
        product = jnp.dot(piece, whole, preferred_element_type=jnp.float32)
        product = product.astype(jnp.bfloat16).reshape(seqs, span, both)
        keys = product[:, :, :key_size].astype(jnp.float32)
        decayed_all.append((weight * key_scale * keys).astype(jnp.bfloat16))
        value_all.append(product[:, :, key_size:])
    decayed = jnp.concatenate(decayed_all, axis=1)
    values = jnp.concatenate(value_all, axis=1)
    partial = jnp.einsum("stk,stv->skv", decayed, values, preferred_element_type=jnp.float32)
    partial_norm = jnp.sum(decayed.astype(jnp.float32), axis=1)

    query_full = new_query.astype(jnp.float32)
    query = lax.dynamic_slice_in_dim(query_full, my_head, 1, 1)[:, 0]
    partial_read = jnp.sum(query[:, :, None] * partial, axis=1)
    summed = jnp.concatenate([partial_read, partial_norm], axis=1)
    board = jnp.zeros((heads,) + summed.shape, jnp.float32)
    board = lax.dynamic_update_slice(board, summed[None], (my_head, 0, 0))
    for mask in token_masks + head_masks:
        board = board + swap(board, mask, count)
    board = jnp.swapaxes(board, 0, 1)
    query_state = board[:, :, :value_size]
    norm = board[:, :, value_size:]
    query_norm = jnp.sum(query_full * norm, axis=-1)

    keep = key_size // count
    held = partial.reshape((seqs,) + (2,) * bits + (keep, value_size))
    axis_of = {1 << b: bits - b for b in range(bits)}
    for mask in token_masks:
        bit = (me // mask) % 2
        axis = axis_of[mask]
        away = lax.dynamic_slice_in_dim(held, 1 - bit, 1, axis).astype(jnp.bfloat16)
        stay = lax.dynamic_slice_in_dim(held, bit, 1, axis)
        held = stay + swap(away, mask, count).astype(jnp.float32)
    held = held.astype(jnp.bfloat16)
    memory = jnp.zeros((seqs, heads, keep, value_size), jnp.bfloat16)
    for off in head_offs:
        piece = held
        for mask in head_masks:
            bit = ((me ^ off) // mask) % 2
            piece = lax.dynamic_slice_in_dim(piece, bit, 1, axis_of[mask])
        piece = piece.reshape(seqs, 1, keep, value_size)
        if off:
            piece = swap(piece, off, count)
        memory = lax.dynamic_update_slice(memory, piece, (0, head_at(off), 0, 0))
    norm_rows = lax.dynamic_slice_in_dim(norm, me * keep, keep, 2)

    forget_new = jax.nn.log_sigmoid(new_gates[1])
    input_new = new_gates[0]
    mixed = jnp.maximum(forget_new + cache_max, input_new)
    carried = jnp.exp(forget_new + cache_max - mixed)
    fresh = jnp.exp(input_new - mixed)
    own_score = jnp.sum(query_full * new_key.astype(jnp.float32), axis=-1) * key_scale
    numer = carried[..., None] * query_state + (fresh * own_score)[..., None] * new_value.astype(
        jnp.float32
    )
    denom = carried * query_norm + fresh * own_score
    first_read = (numer / jnp.maximum(jnp.abs(denom), 1.0)[..., None]).astype(jnp.bfloat16)
    return (memory, norm_rows, cache_max, first_read)


def solution(mesh):
    placed = (
        P(None, "sp", None),
        P("sp", "tp"),
        P("sp", "tp"),
        P(),
        P(),
        P(),
        P(),
        P(None, "tp", None),
        P(None, "tp", None),
        P(None, "tp", None),
        P(None, None, "tp"),
    )
    return jax.shard_map(
        per_device,
        mesh=mesh,
        in_specs=placed,
        out_specs=(
            P(None, "tp", "sp", None),
            P(None, "tp", "sp"),
            P(None, "tp"),
            P(None, "tp", None),
        ),
        check_vma=False,
    )
```

```python
import jax
import jax.numpy as jnp
from jax import lax
from jax.sharding import PartitionSpec as P


def swap(value, mask, count):
    return lax.ppermute(value, "sp", [(i, i ^ mask) for i in range(count)])


def swap_core(value):
    cores = lax.axis_size("tp")
    return lax.ppermute(value, "tp", [(i, cores - 1 - i) for i in range(cores)])


def offsets_of(masks):
    found = [0]
    for mask in masks:
        found = found + [off ^ mask for off in found]
    return found


def spread(value, masks, count):
    held = {0: value}
    for mask in masks:
        for off in list(held):
            held[off ^ mask] = swap(held[off], mask, count)
    return held


def plan(count, heads):
    bits = count.bit_length() - 1
    head_bits = heads.bit_length() - 1
    masks = [1 << b for b in range(bits)]
    preferred = [1 << b for b in range(0, bits, 2)] + [1 << b for b in range(1, bits, 2)]
    head_masks = sorted(preferred[:head_bits])
    token_masks = [m for m in masks if m not in head_masks]
    return head_masks, token_masks


def packed(index, masks):
    total = 0
    for place, mask in enumerate(masks):
        total = total + ((index // mask) % 2) * (1 << place)
    return total


def per_device(
    prompt,
    w_key,
    w_value,
    w_igate,
    w_fgate,
    input_bias,
    forget_bias,
    new_query,
    new_key,
    new_value,
    new_gates,
):
    count = lax.axis_size("sp")
    me = lax.axis_index("sp")
    core = lax.axis_index("tp")
    seqs, span, width = prompt.shape
    heads, key_size = new_query.shape[1:]
    value_size = new_value.shape[2]
    key_scale = key_size ** (-0.5)
    head_masks, token_masks = plan(count, heads)
    head_offs = offsets_of(head_masks)
    my_head = packed(me, head_masks)
    bits = count.bit_length() - 1

    def head_at(off):
        return packed(me ^ off, head_masks)

    depth = w_key.shape[0]
    both = key_size + value_size

    def columns(head):
        keys = lax.dynamic_slice_in_dim(w_key, head * key_size, key_size, 1)
        values = lax.dynamic_slice_in_dim(w_value, head * value_size, value_size, 1)
        return jnp.concatenate([keys, values], axis=1)

    pieces = {}
    for off in head_offs:
        piece = columns(head_at(off))
        pieces[off] = swap(piece, off, count) if off else piece
    own_groups = spread(pieces[0], token_masks[::-1], count)

    rows = prompt.reshape(seqs * span, width)
    w_gates = jnp.concatenate([w_igate, w_fgate], axis=1)
    all_heads = w_igate.shape[1]
    raw = jnp.einsum("dh,td->ht", w_gates, rows, preferred_element_type=jnp.float32)
    bias = jnp.concatenate([input_bias, forget_bias])
    raw = (raw + bias[:, None]).reshape(2, all_heads, seqs, span)
    raw = lax.dynamic_slice_in_dim(raw, core * heads, heads, 1)
    log_forget = jax.nn.log_sigmoid(raw[1])
    until = (
        lax.broadcasted_iota(jnp.int32, (span, span), 0)
        <= lax.broadcasted_iota(jnp.int32, (span, span), 1)
    ).astype(jnp.float32)
    running = jnp.einsum("hst,tu->hsu", log_forget, until, precision=lax.Precision.HIGHEST)
    total = jnp.sum(log_forget, axis=2)
    log_weight = total[:, :, None] - running + raw[0]
    maximum = jnp.max(log_weight, axis=2)

    lane = lax.broadcasted_iota(jnp.int32, (1, 1, 1, count), 3)
    stats = jnp.stack([total, maximum])
    table = jnp.where(lane == me, stats[..., None], 0.0)
    weights = {0: log_weight}
    for mask in head_masks:
        table = table + swap(table, mask, count)
        for off in list(weights):
            weights[off ^ mask] = swap(weights[off], mask, count)

    shared = lax.axis_size("tp") == 2
    half = seqs * span // 2
    mine = lax.dynamic_slice_in_dim(rows, core * half, half, 0) if shared else rows
    ahead = lax.optimization_barrier(
        (mine, table, tuple(weights[off] for off in head_offs), tuple(pieces[off] for off in head_offs))
    )
    mine, table = ahead[0], ahead[1]
    weights = dict(zip(head_offs, ahead[2]))
    pieces = dict(zip(head_offs, ahead[3]))
    halves = {0: mine}
    for mask in head_masks:
        halves[mask] = swap(mine, mask, count)
    groups = {0: own_groups}
    for off in head_offs[1:]:
        groups[off] = spread(pieces[off], token_masks[::-1], count)

    for mask in token_masks:
        table = table + swap(table, mask, count)
    totals, maxima = table[0], table[1]
    above = lax.broadcasted_iota(jnp.int32, (count, count), 1) > lax.broadcasted_iota(
        jnp.int32, (count, count), 0
    )
    later = jnp.sum(jnp.where(above, totals[:, :, None, :], 0.0), axis=-1)
    cache_max = jnp.max(later + maxima, axis=-1)
    shift = later - cache_max[..., None]
    index = lax.broadcasted_iota(jnp.int32, (heads, 1, 1), 0)
    scales = []
    for off in head_offs:
        factor = jnp.sum(jnp.where(lane[0] == (me ^ off), shift, 0.0), axis=-1)
        level = weights[off] + factor[:, :, None]
        level = jnp.sum(jnp.where(index == my_head, level, 0.0), axis=0)
        scales.append(jnp.exp(level) * key_scale)
    scales = jnp.stack(scales)[..., None]
    cache_max = cache_max.T

    for off in head_offs[1:]:
        if off not in halves:
            last = off & -off
            tied = lax.optimization_barrier((halves[off ^ last], scales))
            scales = tied[1]
            halves[off] = swap(tied[0], last, count)
    features = {0: rows}
    for off in head_offs[1:]:
        if not shared:
            features[off] = halves[off]
            continue
        other = swap_core(halves[off])
        first = jnp.where(core == 0, halves[off], other)
        second = jnp.where(core == 0, other, halves[off])
        features[off] = jnp.concatenate([first, second], axis=0)

    whole = jnp.zeros((count * depth, both), jnp.bfloat16)
    for off in head_offs:
        for token_off, piece in groups[off].items():
            whole = lax.dynamic_update_slice(whole, piece, ((me ^ off ^ token_off) * depth, 0))

    decayed_all, value_all = [], []
    for place, off in enumerate(head_offs):
        product = jnp.dot(features[off], whole, preferred_element_type=jnp.float32)
        product = product.astype(jnp.bfloat16).reshape(seqs, span, both)
        keys = product[:, :, :key_size].astype(jnp.float32)
        decayed_all.append((scales[place] * keys).astype(jnp.bfloat16))
        value_all.append(product[:, :, key_size:])
    decayed = jnp.concatenate(decayed_all, axis=1)
    values = jnp.concatenate(value_all, axis=1)
    partial = jnp.einsum("stk,stv->skv", decayed, values, preferred_element_type=jnp.float32)
    partial_norm = jnp.sum(decayed.astype(jnp.float32), axis=1)

    query_full = new_query.astype(jnp.float32)
    query = lax.dynamic_slice_in_dim(query_full, my_head, 1, 1)[:, 0]
    partial_read = jnp.sum(query[:, :, None] * partial, axis=1)
    summed = jnp.concatenate([partial_read, partial_norm], axis=1)
    keep = key_size // count
    held = partial.reshape((seqs,) + (2,) * bits + (keep, value_size))
    axis_of = {1 << b: bits - b for b in range(bits)}
    for mask in token_masks:
        bit = (me // mask) % 2
        axis = axis_of[mask]
        away = lax.dynamic_slice_in_dim(held, 1 - bit, 1, axis).astype(jnp.bfloat16)
        stay = lax.dynamic_slice_in_dim(held, bit, 1, axis)
        came, heard = lax.optimization_barrier(
            (swap(away, mask, count), swap(summed, mask, count))
        )
        held = stay + came.astype(jnp.float32)
        summed = summed + heard
    held = held.astype(jnp.bfloat16)
    memory = jnp.zeros((seqs, heads, keep, value_size), jnp.bfloat16)
    board = jnp.zeros((seqs, heads, summed.shape[1]), jnp.float32)
    for off in head_offs:
        piece = held
        for mask in head_masks:
            bit = ((me ^ off) // mask) % 2
            piece = lax.dynamic_slice_in_dim(piece, bit, 1, axis_of[mask])
        piece = piece.reshape(seqs, 1, keep, value_size)
        spoken = summed[:, None]
        if off:
            piece, spoken = swap(piece, off, count), swap(spoken, off, count)
        memory = lax.dynamic_update_slice(memory, piece, (0, head_at(off), 0, 0))
        board = board + jnp.where(index[None, :, :, 0] == head_at(off), spoken, 0.0)
    query_state = board[:, :, :value_size]
    norm = board[:, :, value_size:]
    query_norm = jnp.sum(query_full * norm, axis=-1)
    norm_rows = lax.dynamic_slice_in_dim(norm, me * keep, keep, 2)

    forget_new = jax.nn.log_sigmoid(new_gates[1])
    input_new = new_gates[0]
    mixed = jnp.maximum(forget_new + cache_max, input_new)
    carried = jnp.exp(forget_new + cache_max - mixed)
    fresh = jnp.exp(input_new - mixed)
    own_score = jnp.sum(query_full * new_key.astype(jnp.float32), axis=-1) * key_scale
    numer = carried[..., None] * query_state + (fresh * own_score)[..., None] * new_value.astype(
        jnp.float32
    )
    denom = carried * query_norm + fresh * own_score
    first_read = (numer / jnp.maximum(jnp.abs(denom), 1.0)[..., None]).astype(jnp.bfloat16)
    return (memory, norm_rows, cache_max, first_read)


def solution(mesh):
    placed = (
        P(None, "sp", None),
        P("sp", "tp"),
        P("sp", "tp"),
        P(),
        P(),
        P(),
        P(),
        P(None, "tp", None),
        P(None, "tp", None),
        P(None, "tp", None),
        P(None, None, "tp"),
    )
    return jax.shard_map(
        per_device,
        mesh=mesh,
        in_specs=placed,
        out_specs=(
            P(None, "tp", "sp", None),
            P(None, "tp", "sp"),
            P(None, "tp"),
            P(None, "tp", None),
        ),
        check_vma=False,
    )
```

```python
import jax
import jax.numpy as jnp
from jax import lax
from jax.sharding import PartitionSpec as P


def swap(value, mask, count):
    return lax.ppermute(value, "sp", [(i, i ^ mask) for i in range(count)])


def swap_core(value):
    cores = lax.axis_size("tp")
    return lax.ppermute(value, "tp", [(i, cores - 1 - i) for i in range(cores)])


def offsets_of(masks):
    found = [0]
    for mask in masks:
        found = found + [off ^ mask for off in found]
    return found


def spread(value, masks, count):
    held = {0: value}
    for mask in masks:
        for off in list(held):
            held[off ^ mask] = swap(held[off], mask, count)
    return held


def plan(count, heads):
    bits = count.bit_length() - 1
    head_bits = heads.bit_length() - 1
    masks = [1 << b for b in range(bits)]
    preferred = [1 << b for b in range(0, bits, 2)] + [1 << b for b in range(1, bits, 2)]
    head_masks = sorted(preferred[:head_bits])
    token_masks = [m for m in masks if m not in head_masks]
    return head_masks, token_masks


def packed(index, masks):
    total = 0
    for place, mask in enumerate(masks):
        total = total + ((index // mask) % 2) * (1 << place)
    return total


def per_device(
    prompt,
    w_key,
    w_value,
    w_igate,
    w_fgate,
    input_bias,
    forget_bias,
    new_query,
    new_key,
    new_value,
    new_gates,
):
    count = lax.axis_size("sp")
    me = lax.axis_index("sp")
    core = lax.axis_index("tp")
    seqs, span, width = prompt.shape
    heads, key_size = new_query.shape[1:]
    value_size = new_value.shape[2]
    key_scale = key_size ** (-0.5)
    head_masks, token_masks = plan(count, heads)
    head_offs = offsets_of(head_masks)
    my_head = packed(me, head_masks)
    bits = count.bit_length() - 1

    def head_at(off):
        return packed(me ^ off, head_masks)

    depth = w_key.shape[0]
    both = key_size + value_size

    def columns(head):
        keys = lax.dynamic_slice_in_dim(w_key, head * key_size, key_size, 1)
        values = lax.dynamic_slice_in_dim(w_value, head * value_size, value_size, 1)
        return jnp.concatenate([keys, values], axis=1)

    rows = prompt.reshape(seqs * span, width)
    sends = tuple(columns(head_at(off)) for off in head_offs)
    sends, rows = lax.optimization_barrier((sends, rows))
    pieces = {}
    for off, piece in zip(head_offs, sends):
        pieces[off] = swap(piece, off, count) if off else piece
    own_groups = spread(pieces[0], token_masks[::-1], count)

    shared = lax.axis_size("tp") == 2
    half = seqs * span // 2
    mine = lax.dynamic_slice_in_dim(rows, core * half, half, 0) if shared else rows
    mine, rows, arrived = lax.optimization_barrier(
        (mine, rows, tuple(pieces[off] for off in head_offs))
    )
    pieces = dict(zip(head_offs, arrived))
    halves = {0: mine}
    for mask in head_masks:
        halves[mask] = swap(mine, mask, count)
    groups = {0: own_groups}
    for off in head_offs[1:]:
        groups[off] = spread(pieces[off], token_masks[::-1], count)

    w_gates = jnp.concatenate([w_igate, w_fgate], axis=1)
    all_heads = w_igate.shape[1]
    raw = jnp.einsum("dh,td->ht", w_gates, rows, preferred_element_type=jnp.float32)
    bias = jnp.concatenate([input_bias, forget_bias])
    raw = (raw + bias[:, None]).reshape(2, all_heads, seqs, span)
    raw = lax.dynamic_slice_in_dim(raw, core * heads, heads, 1)
    log_forget = jax.nn.log_sigmoid(raw[1])
    until = (
        lax.broadcasted_iota(jnp.int32, (span, span), 0)
        <= lax.broadcasted_iota(jnp.int32, (span, span), 1)
    ).astype(jnp.float32)
    running = jnp.einsum("hst,tu->hsu", log_forget, until, precision=lax.Precision.HIGHEST)
    total = jnp.sum(log_forget, axis=2)
    log_weight = total[:, :, None] - running + raw[0]
    maximum = jnp.max(log_weight, axis=2)

    lane = lax.broadcasted_iota(jnp.int32, (1, 1, 1, count), 3)
    message = jnp.concatenate([log_weight, total[..., None], maximum[..., None]], axis=2)
    told = tuple(swap(message, off, count) if off else message for off in head_offs)

    weights, table = {}, 0.0
    for off, heard in zip(head_offs, told):
        weights[off] = heard[:, :, :span]
        stats = jnp.stack([heard[:, :, span], heard[:, :, span + 1]])
        table = table + jnp.where(lane == (me ^ off), stats[..., None], 0.0)
    for mask in token_masks:
        table = table + swap(table, mask, count)
    totals, maxima = table[0], table[1]
    above = lax.broadcasted_iota(jnp.int32, (count, count), 1) > lax.broadcasted_iota(
        jnp.int32, (count, count), 0
    )
    later = jnp.sum(jnp.where(above, totals[:, :, None, :], 0.0), axis=-1)
    cache_max = jnp.max(later + maxima, axis=-1)
    shift = later - cache_max[..., None]
    index = lax.broadcasted_iota(jnp.int32, (heads, 1, 1), 0)
    scales = []
    for off in head_offs:
        factor = jnp.sum(jnp.where(lane[0] == (me ^ off), shift, 0.0), axis=-1)
        level = weights[off] + factor[:, :, None]
        level = jnp.sum(jnp.where(index == my_head, level, 0.0), axis=0)
        scales.append(jnp.exp(level) * key_scale)
    scales = jnp.stack(scales)[..., None]
    cache_max = cache_max.T

    for off in head_offs[1:]:
        if off not in halves:
            last = off & -off
            halves[off] = swap(halves[off ^ last], last, count)
    features = {0: rows}
    for off in head_offs[1:]:
        if not shared:
            features[off] = halves[off]
            continue
        if off == head_offs[-1]:
            halves[off], scales = lax.optimization_barrier((halves[off], scales))
        other = swap_core(halves[off])
        first = jnp.where(core == 0, halves[off], other)
        second = jnp.where(core == 0, other, halves[off])
        features[off] = jnp.concatenate([first, second], axis=0)

    whole = jnp.zeros((count * depth, both), jnp.bfloat16)
    for off in head_offs:
        for token_off, piece in groups[off].items():
            whole = lax.dynamic_update_slice(whole, piece, ((me ^ off ^ token_off) * depth, 0))

    decayed_all, value_all = [], []
    for place, off in enumerate(head_offs):
        product = jnp.dot(features[off], whole, preferred_element_type=jnp.float32)
        product = product.astype(jnp.bfloat16).reshape(seqs, span, both)
        keys = product[:, :, :key_size].astype(jnp.float32)
        decayed_all.append((scales[place] * keys).astype(jnp.bfloat16))
        value_all.append(product[:, :, key_size:])
    decayed = jnp.concatenate(decayed_all, axis=1)
    values = jnp.concatenate(value_all, axis=1)
    partial = jnp.einsum("stk,stv->skv", decayed, values, preferred_element_type=jnp.float32)
    partial_norm = jnp.sum(decayed.astype(jnp.float32), axis=1)

    query_full = new_query.astype(jnp.float32)
    query = lax.dynamic_slice_in_dim(query_full, my_head, 1, 1)[:, 0]
    partial_read = jnp.sum(query[:, :, None] * partial, axis=1)
    summed = jnp.concatenate([partial_read, partial_norm], axis=1)
    keep = key_size // count
    held = partial.reshape((seqs,) + (2,) * bits + (keep, value_size))
    axis_of = {1 << b: bits - b for b in range(bits)}
    for mask in token_masks:
        bit = (me // mask) % 2
        axis = axis_of[mask]
        away = lax.dynamic_slice_in_dim(held, 1 - bit, 1, axis).astype(jnp.bfloat16)
        stay = lax.dynamic_slice_in_dim(held, bit, 1, axis)
        came, heard = lax.optimization_barrier(
            (swap(away, mask, count), swap(summed, mask, count))
        )
        held = stay + came.astype(jnp.float32)
        summed = summed + heard
    held = held.astype(jnp.bfloat16)
    memory = jnp.zeros((seqs, heads, keep, value_size), jnp.bfloat16)
    board = jnp.zeros((seqs, heads, summed.shape[1]), jnp.float32)
    for off in head_offs:
        piece = held
        for mask in head_masks:
            bit = ((me ^ off) // mask) % 2
            piece = lax.dynamic_slice_in_dim(piece, bit, 1, axis_of[mask])
        piece = piece.reshape(seqs, 1, keep, value_size)
        spoken = summed[:, None]
        if off:
            piece, spoken = swap(piece, off, count), swap(spoken, off, count)
        memory = lax.dynamic_update_slice(memory, piece, (0, head_at(off), 0, 0))
        board = board + jnp.where(index[None, :, :, 0] == head_at(off), spoken, 0.0)
    query_state = board[:, :, :value_size]
    norm = board[:, :, value_size:]
    query_norm = jnp.sum(query_full * norm, axis=-1)
    norm_rows = lax.dynamic_slice_in_dim(norm, me * keep, keep, 2)

    forget_new = jax.nn.log_sigmoid(new_gates[1])
    input_new = new_gates[0]
    mixed = jnp.maximum(forget_new + cache_max, input_new)
    carried = jnp.exp(forget_new + cache_max - mixed)
    fresh = jnp.exp(input_new - mixed)
    own_score = jnp.sum(query_full * new_key.astype(jnp.float32), axis=-1) * key_scale
    numer = carried[..., None] * query_state + (fresh * own_score)[..., None] * new_value.astype(
        jnp.float32
    )
    denom = carried * query_norm + fresh * own_score
    first_read = (numer / jnp.maximum(jnp.abs(denom), 1.0)[..., None]).astype(jnp.bfloat16)
    return (memory, norm_rows, cache_max, first_read)


def solution(mesh):
    placed = (
        P(None, "sp", None),
        P("sp", "tp"),
        P("sp", "tp"),
        P(),
        P(),
        P(),
        P(),
        P(None, "tp", None),
        P(None, "tp", None),
        P(None, "tp", None),
        P(None, None, "tp"),
    )
    return jax.shard_map(
        per_device,
        mesh=mesh,
        in_specs=placed,
        out_specs=(
            P(None, "tp", "sp", None),
            P(None, "tp", "sp"),
            P(None, "tp"),
            P(None, "tp", None),
        ),
        check_vma=False,
    )
```
